32 devices in a mesh: ep: 8 (over z, x), tp: 4 (over y, core).
Axes of the slice: x: 2, y: 2, z: 4, core: 2. Of those that a mesh axis runs over, the one named last changes fastest.
Arguments:
- tokens: bfloat16 [1024, 2048], P('ep'), may hold values from -6 to 6
- cotangent: bfloat16 [1024, 2048], P('ep'), may hold values from -1.5 to 1.5
- routes: int32 [1024, 2], P('ep'), may hold values from 0 to 3, all different within a row; in each aligned block of 128 rows (0 to 127, 128 to 255, ...) at most 96 rows name the same one
- router: bfloat16 [2048, 4], replicated, may hold values from -0.125 to 0.125
- w_gate: bfloat16 [8, 2048, 2048], P('ep', None, 'tp'), may hold values from -0.125 to 0.125
- w_up: bfloat16 [8, 2048, 2048], P('ep', None, 'tp'), may hold values from -0.125 to 0.125
- w_down: bfloat16 [8, 2048, 2048], P('ep', 'tp'), may hold values from -0.09375 to 0.09375
Outputs:
- token_grad: bfloat16 [1024, 2048], P('ep', 'tp')
- gate_grad: float32 [1024, 2], P('ep')
- grad_gate: bfloat16 [8, 2048, 2048], P('ep', None, 'tp')
- grad_up: bfloat16 [8, 2048, 2048], P('ep', None, 'tp')
- grad_down: bfloat16 [8, 2048, 2048], P('ep', 'tp')
- router_grad: float32 [2048, 4], P(('ep', 'tp'))
The draws below stay inside these ranges and needn't reach their ends.
Inputs may be any that keep to these rules, and one draw needn't show every extreme that they name: `routes`: each row names 2 different experts. In the rows of one index of ep (aligned blocks of 128 rows) no expert is named by more than 96 rows, a bound that some block reaches.
All inputs are finite; a program needn't handle non-finite values.
Results may differ from the reference program's by a relative error of at most 0.018.
Values may be sent and summed in bfloat16 or wider, within the bound.
No kernel may reach another device: no remote copies, remote signals or barrier semaphores. Data moves between devices by JAX's collectives and lax.ppermute only.
A program may use at most 64 MiB of HBM per device.

```python
import math
import jax
import jax.numpy as jnp
import numpy as np
from jax import lax

D = 2048
FF = 4096
TOP = 2
BLOCKS = 2
TOK_EP = 128
EXPERTS = 4
TOKENS = 1024
CAP = 96
N_EP = 8
N_TP = 4


def spiked(values, key, source, target, parts, factor):
    owner, partner = [(jnp.arange(values.shape[axis_at]) // (values.shape[axis_at] // parts)).reshape([-1 if axis == axis_at else 1 for axis in range(values.ndim)]) for axis_at in (source, target)]
    chosen = jax.random.permutation(key, parts)[partner]
    strong = (owner == chosen) | (owner == (partner + parts // 2) % parts)
    return jnp.where(strong, factor * values, values)


def block_levels(stream_key, dims, pieces, least, top_value):
    def one(dim, blocks):
        steps = jax.random.uniform(jax.random.fold_in(jax.random.fold_in(stream_key, 6), dim), (blocks,), jnp.float32, least / len(pieces), top_value / len(pieces))
        return jnp.repeat(jnp.exp(steps), dims[dim] // blocks).reshape((-1,) + (1,) * (len(dims) - dim - 1))

    level = one(*pieces[0])
    for cut in pieces[1:]:
        level = level * one(*cut)
    return level


def routed_block(key, own, number, rows, number_of, top, limit, slope):
    sequence = jax.random.permutation(key, number_of)
    heavy_load, ordinary = load_shares(number_of, rows * top, limit, slope, True), load_shares(number_of, rows * top, limit, slope, False)
    places = jnp.arange(number_of)

    def named(sizes, turn):
        used = int((sizes > 0).sum())
        fixed = max(1, used // 4)
        shifted = fixed + (places - fixed + turn * (used - fixed)) % max(1, number_of - fixed)
        return jnp.zeros((number_of,), jnp.int32).at[sequence[jnp.where(places < fixed, places, shifted)]].set(jnp.asarray(sizes, jnp.int32))

    sizes = jnp.where(number % 4 == 0, named(heavy_load, number // 4), named(ordinary, number - number // 4 - 1))
    mixed = jax.random.permutation(jax.random.fold_in(own, 3), number_of)
    giver, taker = mixed[0:number_of // 2 * 2:2], mixed[1:number_of // 2 * 2:2]
    slack = jnp.minimum(sizes[giver] - 1, limit - sizes[taker]) // 2
    slack = jnp.where((giver == sequence[0]) | (taker == sequence[0]) | (sizes[taker] == 0), 0, jnp.maximum(slack, 0))
    shifted = jax.random.randint(jax.random.fold_in(own, 4), (number_of // 2,), 0, 1 << 20) % (slack + 1)
    sizes = sizes.at[giver].add(-shifted).at[taker].add(shifted)
    members = jnp.searchsorted(jnp.cumsum(sizes), jnp.arange(rows * top), side="right").astype(jnp.int32)
    table = members.reshape(top, rows).T
    table = table[jax.random.permutation(jax.random.fold_in(own, 1), rows)]
    turn = jax.random.randint(jax.random.fold_in(own, 2), (rows, 1), 0, top)
    return jnp.take_along_axis(table, (jnp.arange(top)[None, :] + turn) % top, axis=1)


def load_shares(number_of, total, most, lean, full):
    loads = [(1 << 20) // math.isqrt(standing ** lean) + 1 for standing in range(1, number_of + 1)]
    largest = most if full else min(most, max(-(-total // number_of), total * loads[0] // sum(loads)))
    least = 1 if total - largest >= number_of - 1 else 0
    holding, spare = [largest] + [least] * (number_of - 1), total - largest - least * (number_of - 1)
    while spare > 0:
        candidates = [i for i in range(1, number_of) if holding[i] < largest] or [i for i in range(1, number_of) if holding[i] < most]
        pool, left = sum([loads[i] for i in candidates]), spare
        for i in candidates:
            addition = min(most - holding[i], max(1, left * loads[i] // pool), spare)
            holding[i] = holding[i] + addition
            spare = spare - addition
    return np.array(holding)


def scatter_about(own_key, extent, spread, most, split=(), kind=jnp.bfloat16):
    drawn = spread * jax.random.normal(own_key, extent, jnp.float32)
    if split:
        drawn = drawn * block_levels(own_key, extent, split, -0.22, 0.18)
    return jnp.clip(drawn, -most, most).astype(kind)


def heavy_noise(rng, shape, deviation, bound, split, heavy, kind=jnp.bfloat16):
    entries = deviation * jax.random.normal(rng, shape, jnp.float32)
    if split:
        entries = entries * block_levels(rng, shape, split, -0.22, 0.18)
    return jnp.clip(spiked(entries, jax.random.fold_in(rng, 3), *heavy), -bound, bound).astype(kind)


def setup_inputs(seed: int = 0) -> dict:
    seeds = jax.random.split(jax.random.key(seed), 8)
    tokens = heavy_noise(seeds[0], (TOKENS, D), 1.0, 6.0, ((0, 8),), (0, 1, 8, 2.0))
    cotangent = scatter_about(seeds[1], (TOKENS, D), 0.25, 1.5, ((0, 8),))
    routes_keys = jax.random.split(jax.random.fold_in(seeds[2], 1), TOKENS // TOK_EP)
    routes_turns = jax.random.permutation(jax.random.fold_in(seeds[2], 3), TOKENS // TOK_EP)
    routes = jax.vmap(lambda own, number: routed_block(jax.random.fold_in(seeds[2], 2), own, number, TOK_EP, EXPERTS, TOP, CAP, 2))(routes_keys, routes_turns).reshape((TOKENS, TOP))
    router = scatter_about(seeds[3], (D, EXPERTS), D ** -0.5, 0.125)
    w_gate = scatter_about(seeds[4], (EXPERTS * BLOCKS, D, FF // BLOCKS), D ** -0.5, 0.125, ((0, 8), (2, 4)))
    w_up = scatter_about(seeds[5], (EXPERTS * BLOCKS, D, FF // BLOCKS), D ** -0.5, 0.125, ((0, 8), (2, 4)))
    w_down = scatter_about(seeds[6], (EXPERTS * BLOCKS, FF // BLOCKS, D), FF ** -0.5, 0.09375, ((0, 8), (1, 4)))
    return {"tokens": tokens, "cotangent": cotangent, "routes": routes, "router": router, "w_gate": w_gate, "w_up": w_up, "w_down": w_down}


def build_slots(block_routes, experts, capacity):
    flat_routes = block_routes.reshape(-1)
    labels = jnp.arange(experts, dtype=jnp.int32)
    hit_mask = (flat_routes[None, :] == labels[:, None]).astype(jnp.int32)
    rank_in = jnp.cumsum(hit_mask, axis=1, dtype=jnp.int32) - 1
    slot_ids = jnp.arange(capacity, dtype=jnp.int32)
    assigned = (hit_mask[:, None, :] == 1) & (rank_in[:, None, :] == slot_ids[None, :, None])
    return assigned.astype(jnp.float32)


def gate_pair(tokens, routes, router, experts):
    logits = jnp.dot(tokens, router, preferred_element_type=jnp.float32)
    labels = jnp.arange(experts, dtype=jnp.int32)
    picked = (routes[:, :, None] == labels[None, None, :]).astype(jnp.float32)
    chosen = jnp.sum(picked * logits[:, None, :], axis=2)
    margin = chosen[:, 0] - chosen[:, 1]
    weights = jnp.stack([jax.nn.sigmoid(margin), jax.nn.sigmoid(-margin)], axis=1)
    return picked, weights


def logit_grads(picked, weights, gate_grad):
    lead_grad = weights[:, 0] * weights[:, 1] * (gate_grad[:, 0] - gate_grad[:, 1])
    pair_grad = jnp.stack([lead_grad, -lead_grad], axis=1)
    return jnp.sum(picked * pair_grad[:, :, None], axis=1)


def expert_grads(rows_in, cot_in, gate_in, gate_weight, up_weight, down_weight):
    pre_gate = jnp.dot(rows_in, gate_weight, preferred_element_type=jnp.float32)
    pre_up = jnp.dot(rows_in, up_weight, preferred_element_type=jnp.float32)
    back_grad = lax.dot_general(cot_in, down_weight, (((1,), (1,)), ((), ())), preferred_element_type=jnp.float32)
    sig_gate = jax.nn.sigmoid(pre_gate)
    active = pre_gate * sig_gate
    hidden = (active * pre_up).astype(jnp.bfloat16)
    gate_terms = jnp.sum(hidden.astype(jnp.float32) * back_grad, axis=1)
    gate_col = gate_in.astype(jnp.float32)[:, None]
    scaled_back = gate_col * back_grad
    d_gate = (scaled_back * pre_up * sig_gate * (1.0 + pre_gate * (1.0 - sig_gate))).astype(jnp.bfloat16)
    d_up = (scaled_back * active).astype(jnp.bfloat16)
    scaled_cot = (gate_col * cot_in.astype(jnp.float32)).astype(jnp.bfloat16)
    contract_rows = (((0,), (0,)), ((), ()))
    grad_gate = lax.dot_general(rows_in, d_gate, contract_rows, preferred_element_type=jnp.float32).astype(jnp.bfloat16)
    grad_up = lax.dot_general(rows_in, d_up, contract_rows, preferred_element_type=jnp.float32).astype(jnp.bfloat16)
    grad_down = lax.dot_general(hidden, scaled_cot, contract_rows, preferred_element_type=jnp.float32).astype(jnp.bfloat16)
    return d_gate, d_up, gate_terms, grad_gate, grad_up, grad_down


def reference(tokens, cotangent, routes, router, w_gate, w_up, w_down):
    highest = lax.Precision.HIGHEST
    picked, weights = gate_pair(tokens, routes, router, EXPERTS)
    gate_send = lax.optimization_barrier(weights.astype(jnp.bfloat16)).astype(jnp.float32)
    assigned = jax.vmap(lambda block_routes: build_slots(block_routes, EXPERTS, CAP))(routes.reshape(N_EP, TOK_EP, TOP))
    by_expert = jnp.transpose(assigned, (1, 0, 2, 3))
    tok_src = tokens.reshape(N_EP, TOK_EP, D).astype(jnp.float32)
    cot_src = cotangent.reshape(N_EP, TOK_EP, D).astype(jnp.float32)
    gate_src = gate_send.reshape(N_EP, TOK_EP * TOP)
    half_ff = FF // BLOCKS
    gate_full = jnp.transpose(w_gate.reshape(EXPERTS, BLOCKS, D, half_ff), (0, 2, 1, 3)).reshape(EXPERTS, D, FF)
    up_full = jnp.transpose(w_up.reshape(EXPERTS, BLOCKS, D, half_ff), (0, 2, 1, 3)).reshape(EXPERTS, D, FF)
    down_full = w_down.reshape(EXPERTS, FF, D)
    nblocks = BLOCKS * N_TP
    block_width = FF // nblocks

    def one_expert(carry, inputs):
        dx_acc, gate_acc = carry
        slots_here, gate_weight, up_weight, down_weight = inputs
        per_token = jnp.sum(slots_here.reshape(N_EP, CAP, TOK_EP, TOP), axis=3)
        rows_in = jnp.einsum('sct,std->scd', per_token, tok_src, precision=highest).astype(jnp.bfloat16).reshape(-1, D)
        cot_in = jnp.einsum('sct,std->scd', per_token, cot_src, precision=highest).astype(jnp.bfloat16).reshape(-1, D)
        gate_in = jnp.einsum('scj,sj->sc', slots_here, gate_src, precision=highest).astype(jnp.bfloat16).reshape(-1)
        d_gate, d_up, gate_terms, grad_gate, grad_up, grad_down = expert_grads(rows_in, cot_in, gate_in, gate_weight, up_weight, down_weight)
        blocks_gate = jnp.einsum('rbh,dbh->rbd', d_gate.astype(jnp.float32).reshape(-1, nblocks, block_width),
                                 gate_weight.astype(jnp.float32).reshape(D, nblocks, block_width))
        blocks_up = jnp.einsum('rbh,dbh->rbd', d_up.astype(jnp.float32).reshape(-1, nblocks, block_width),
                               up_weight.astype(jnp.float32).reshape(D, nblocks, block_width))
        block_dx = lax.optimization_barrier((blocks_gate + blocks_up).astype(jnp.bfloat16)).astype(jnp.float32)
        pair_dx = jnp.sum(block_dx, axis=1).reshape(N_EP, CAP, D)
        dx_acc = dx_acc + jnp.einsum('sct,scd->std', per_token, pair_dx, precision=highest)
        gate_acc = gate_acc + jnp.einsum('scj,sc->sj', slots_here, gate_terms.reshape(N_EP, CAP), precision=highest)
        return (dx_acc, gate_acc), (grad_gate, grad_up, grad_down)

    start_carry = (jnp.zeros((N_EP, TOK_EP, D), jnp.float32), jnp.zeros((N_EP, TOK_EP * TOP), jnp.float32))
    (dx_acc, gate_acc), (all_gate, all_up, all_down) = lax.scan(one_expert, start_carry, (by_expert, gate_full, up_full, down_full))
    gate_grad = gate_acc.reshape(TOKENS, TOP)
    logit_grad = logit_grads(picked, weights, gate_grad)
    router_grad = jnp.dot(tokens.astype(jnp.float32).T, logit_grad, precision=highest)
    token_grad = (dx_acc.reshape(TOKENS, D) + jnp.dot(logit_grad, router.astype(jnp.float32).T, precision=highest)).astype(jnp.bfloat16)
    grad_gate = jnp.transpose(all_gate.reshape(EXPERTS, D, BLOCKS, half_ff), (0, 2, 1, 3)).reshape(EXPERTS * BLOCKS, D, half_ff)
    grad_up = jnp.transpose(all_up.reshape(EXPERTS, D, BLOCKS, half_ff), (0, 2, 1, 3)).reshape(EXPERTS * BLOCKS, D, half_ff)
    grad_down = all_down.reshape(EXPERTS * BLOCKS, half_ff, D)
    return (token_grad, gate_grad, grad_gate, grad_up, grad_down, router_grad)
```

```python
import jax
import jax.numpy as jnp
from jax import lax
from jax.sharding import PartitionSpec as P

BLOCKS = 2


def build_slots(block_routes, experts, capacity):
    flat_routes = block_routes.reshape(-1)
    labels = jnp.arange(experts, dtype=jnp.int32)
    hit_mask = (flat_routes[None, :] == labels[:, None]).astype(jnp.int32)
    rank_in = jnp.cumsum(hit_mask, axis=1, dtype=jnp.int32) - 1
    slot_ids = jnp.arange(capacity, dtype=jnp.int32)
    assigned = (hit_mask[:, None, :] == 1) & (rank_in[:, None, :] == slot_ids[None, :, None])
    return assigned.astype(jnp.float32)


def gate_pair(tokens, routes, router, experts):
    logits = jnp.dot(tokens, router, preferred_element_type=jnp.float32)
    labels = jnp.arange(experts, dtype=jnp.int32)
    picked = (routes[:, :, None] == labels[None, None, :]).astype(jnp.float32)
    chosen = jnp.sum(picked * logits[:, None, :], axis=2)
    margin = chosen[:, 0] - chosen[:, 1]
    weights = jnp.stack([jax.nn.sigmoid(margin), jax.nn.sigmoid(-margin)], axis=1)
    return (picked, weights)


def logit_grads(picked, weights, gate_grad):
    lead_grad = weights[:, 0] * weights[:, 1] * (gate_grad[:, 0] - gate_grad[:, 1])
    pair_grad = jnp.stack([lead_grad, -lead_grad], axis=1)
    return jnp.sum(picked * pair_grad[:, :, None], axis=1)


def expert_grads(rows_in, cot_in, gate_in, gate_weight, up_weight, down_weight):
    pre_gate = jnp.dot(rows_in, gate_weight, preferred_element_type=jnp.float32)
    pre_up = jnp.dot(rows_in, up_weight, preferred_element_type=jnp.float32)
    back_grad = lax.dot_general(
        cot_in, down_weight, (((1,), (1,)), ((), ())), preferred_element_type=jnp.float32
    )
    sig_gate = jax.nn.sigmoid(pre_gate)
    active = pre_gate * sig_gate
    hidden = (active * pre_up).astype(jnp.bfloat16)
    gate_terms = jnp.sum(hidden.astype(jnp.float32) * back_grad, axis=1)
    gate_col = gate_in.astype(jnp.float32)[:, None]
    scaled_back = gate_col * back_grad
    d_gate = (scaled_back * pre_up * sig_gate * (1.0 + pre_gate * (1.0 - sig_gate))).astype(
        jnp.bfloat16
    )
    d_up = (scaled_back * active).astype(jnp.bfloat16)
    scaled_cot = (gate_col * cot_in.astype(jnp.float32)).astype(jnp.bfloat16)
    contract_rows = (((0,), (0,)), ((), ()))
    grad_gate = lax.dot_general(
        rows_in, d_gate, contract_rows, preferred_element_type=jnp.float32
    ).astype(jnp.bfloat16)
    grad_up = lax.dot_general(
        rows_in, d_up, contract_rows, preferred_element_type=jnp.float32
    ).astype(jnp.bfloat16)
    grad_down = lax.dot_general(
        hidden, scaled_cot, contract_rows, preferred_element_type=jnp.float32
    ).astype(jnp.bfloat16)
    return (d_gate, d_up, gate_terms, grad_gate, grad_up, grad_down)


def spread_slabs(packed, experts, slab_count):
    widened = jnp.broadcast_to(packed[:, None], (experts, BLOCKS) + packed.shape[1:])
    return widened.reshape((slab_count,) + packed.shape[1:])


def shards(tokens, cotangent, routes, router, w_gate, w_up, w_down):
    highest = lax.Precision.HIGHEST
    ep_count = lax.axis_size("ep")
    tp_count = lax.axis_size("tp")
    experts = ep_count // BLOCKS
    tok_rows, width = tokens.shape
    top_count = routes.shape[1]
    capacity = 3 * tok_rows * top_count // (2 * experts)
    col_width = width // tp_count
    tp_index = lax.axis_index("tp")
    picked, weights = gate_pair(tokens, routes, router, experts)
    assigned = build_slots(routes, experts, capacity)
    per_token = jnp.sum(assigned.reshape(experts, capacity, tok_rows, top_count), axis=3)
    token_map = per_token.astype(jnp.bfloat16)
    gate_send = weights.astype(jnp.bfloat16)
    gate_slots = jnp.einsum(
        "ecj,j->ec", assigned, gate_send.astype(jnp.float32).reshape(-1), precision=highest
    ).astype(jnp.bfloat16)
    gate_out = spread_slabs(gate_slots, experts, ep_count)

    def pack_rows(source):
        packed = jnp.einsum(
            "ect,td->ecd", token_map, source, preferred_element_type=jnp.float32
        ).astype(jnp.bfloat16)
        return spread_slabs(packed, experts, ep_count)

    tok_part = lax.dynamic_slice_in_dim(tokens, tp_index * col_width, col_width, 1)
    cot_part = lax.dynamic_slice_in_dim(cotangent, tp_index * col_width, col_width, 1)
    recv_part, recv_cot_part, recv_gate = (
        lax.all_to_all(pack_rows(tok_part), "ep", split_axis=0, concat_axis=0, tiled=True),
        lax.all_to_all(pack_rows(cot_part), "ep", split_axis=0, concat_axis=0, tiled=True),
        lax.all_to_all(gate_out, "ep", split_axis=0, concat_axis=0, tiled=True),
    )
    recv_rows, recv_cot = (
        lax.all_gather(recv_part, "tp", axis=2, tiled=True),
        lax.all_gather(recv_cot_part, "tp", axis=2, tiled=True),
    )
    rows_in = recv_rows.reshape(-1, width)
    cot_in = recv_cot.reshape(-1, width)
    gate_in = recv_gate.reshape(-1)
    d_gate, d_up, gate_terms, grad_gate, grad_up, grad_down = expert_grads(
        rows_in, cot_in, gate_in, w_gate[0], w_up[0], w_down[0]
    )
    contract_hidden = (((1,), (1,)), ((), ()))
    partial_dx = lax.dot_general(
        d_gate, w_gate[0], contract_hidden, preferred_element_type=jnp.float32
    )
    partial_dx = partial_dx + lax.dot_general(
        d_up, w_up[0], contract_hidden, preferred_element_type=jnp.float32
    )
    summed_dx = lax.psum_scatter(
        partial_dx.reshape(ep_count, capacity, width).astype(jnp.bfloat16),
        "tp",
        scatter_dimension=2,
        tiled=True,
    ).astype(jnp.float32)
    gate_sums = lax.psum(gate_terms.reshape(ep_count, capacity), "tp")
    back_dx, back_gate = (
        lax.all_to_all(
            summed_dx.astype(jnp.bfloat16), "ep", split_axis=0, concat_axis=0, tiled=True
        ).astype(summed_dx.dtype),
        lax.all_to_all(
            gate_sums.astype(jnp.bfloat16), "ep", split_axis=0, concat_axis=0, tiled=True
        ).astype(gate_sums.dtype),
    )
    slab_dx = jnp.sum(back_dx.reshape(experts, BLOCKS, capacity, col_width), axis=1)
    routed_dx = jnp.einsum("ect,ecd->td", per_token, slab_dx, precision=highest)
    slab_gate = jnp.sum(back_gate.reshape(experts, BLOCKS, capacity), axis=1)
    gate_grad = jnp.einsum("ecj,ec->j", assigned, slab_gate, precision=highest).reshape(
        tok_rows, top_count
    )
    logit_grad = logit_grads(picked, weights, gate_grad)
    router_cols = lax.dynamic_slice_in_dim(router, tp_index * col_width, col_width, 0).astype(
        jnp.float32
    )
    token_grad = (routed_dx + jnp.dot(logit_grad, router_cols.T, precision=highest)).astype(
        jnp.bfloat16
    )
    seg_rows = tok_rows // tp_count
    own_rows = lax.dynamic_slice_in_dim(tokens, tp_index * seg_rows, seg_rows, 0).astype(
        jnp.float32
    )
    own_logit = lax.dynamic_slice_in_dim(logit_grad, tp_index * seg_rows, seg_rows, 0)
    router_grad = lax.psum_scatter(
        jnp.dot(own_rows.T, own_logit, precision=highest),
        ("ep", "tp"),
        scatter_dimension=0,
        tiled=True,
    )
    return (token_grad, gate_grad, grad_gate[None], grad_up[None], grad_down[None], router_grad)

def fast_shards(tokens, cotangent, routes, router, w_gate, w_up, w_down):
    f32, bf16 = jnp.float32, jnp.bfloat16
    highest = lax.Precision.HIGHEST
    axes = ("ep", "tp")
    ep_count = lax.axis_size("ep")
    tp_count = lax.axis_size("tp")
    total = ep_count * tp_count
    experts = ep_count // BLOCKS
    rows, width = tokens.shape
    top = routes.shape[1]
    cap = 3 * rows * top // (2 * experts)
    quarter = width // tp_count
    hid = w_gate.shape[2]
    ep = lax.axis_index("ep")
    tp = lax.axis_index("tp")
    here = ep // BLOCKS
    core = tp % 2
    pad = 8

    def swap(value, bits):
        return lax.ppermute(value, axes, [(i, i ^ bits) for i in range(total)])

    def mixed(value, bits_even, bits_odd):
        return lax.ppermute(
            value, axes, [(i, i ^ (bits_odd if i % 2 else bits_even)) for i in range(total)]
        )

    cbit, ybit, xbit, zbit = 1, 2, tp_count, tp_count * BLOCKS

    logits = jnp.dot(tokens, router, preferred_element_type=f32)
    labels = jnp.arange(experts, dtype=jnp.int32)
    picked = (routes[:, :, None] == labels[None, None, :]).astype(f32)
    chosen = jnp.sum(picked * logits[:, None, :], axis=2)
    margin = chosen[:, 0] - chosen[:, 1]
    weights = jnp.stack([jax.nn.sigmoid(margin), jax.nn.sigmoid(-margin)], axis=1)
    product = weights[:, 0] * weights[:, 1]
    near = here ^ labels
    hit = jnp.any(routes[None] == near[:, None, None], axis=2)
    lower = (jnp.arange(rows)[:, None] <= jnp.arange(rows)[None, :]).astype(bf16)
    rank = jnp.dot(hit.astype(bf16), lower, preferred_element_type=f32).astype(jnp.int32) - 1
    slots = jnp.arange(cap, dtype=jnp.int32)
    place = (hit[:, None, :] & (rank[:, None, :] == slots[None, :, None])).astype(bf16)
    first = routes[None, :, 0] == near[:, None]
    gate_tok = jnp.where(first, weights[None, :, 0], weights[None, :, 1]).astype(bf16)
    other_tok = jnp.where(first, routes[None, :, 1], routes[None, :, 0]).astype(bf16)
    prod_hi = product.astype(bf16)
    prod_lo = (product - prod_hi.astype(f32)).astype(bf16)
    flat = jnp.broadcast_to(prod_hi[None], gate_tok.shape), jnp.broadcast_to(prod_lo[None], gate_tok.shape)
    meta_tok = jnp.stack([gate_tok, flat[0], flat[1], other_tok], axis=1)
    meta = jnp.einsum("jkt,jct->jkc", meta_tok, place, preferred_element_type=f32).astype(bf16)
    meta = jnp.pad(meta, ((0, 0), (0, pad - meta.shape[1]), (0, 2 * quarter - cap)))
    source = jnp.concatenate(
        [
            lax.dynamic_slice_in_dim(tokens, tp * quarter, quarter, 1),
            lax.dynamic_slice_in_dim(cotangent, tp * quarter, quarter, 1),
        ],
        axis=1,
    )
    packed = jnp.einsum("jct,td->jcd", place, source, preferred_element_type=f32).astype(bf16)
    packed = jnp.concatenate([packed, meta], axis=1)

    turn = tp ^ jnp.arange(tp_count)
    wg = w_gate[0].reshape(tp_count, quarter, hid)[turn].reshape(width, hid)
    wu = w_up[0].reshape(tp_count, quarter, hid)[turn].reshape(width, hid)
    wd = w_down[0].reshape(hid, tp_count, quarter)[:, turn].reshape(hid, width)

    half = experts // 2
    pieces = [list(range(half)), list(range(half, experts))]
    kept, backs = [], [None] * experts
    for piece in pieces:
        got = [packed[j] if j == 0 else swap(packed[j], zbit * j) for j in piece]
        own = jnp.stack(got)
        side = swap(own, xbit)
        over = swap(own, ybit)
        diag = mixed(jnp.where(core == 0, side, over), ybit, xbit)
        blocks = jnp.stack([own, side, over, diag])
        twin = swap(blocks, cbit)

        def merge(which):
            return jnp.stack(
                [
                    jnp.concatenate([which(blocks[0]), which(twin[0]), which(blocks[2]), which(twin[2])], axis=-1),
                    jnp.concatenate([which(blocks[1]), which(twin[1]), which(blocks[3]), which(twin[3])], axis=-1),
                ]
            ).reshape(-1, width)

        x_in = merge(lambda v: v[:, :cap, :quarter])
        c_in = merge(lambda v: v[:, :cap, quarter:])
        info = jnp.stack([own[:, cap:, :cap], side[:, cap:, :cap]]).astype(f32)
        info = jnp.transpose(info, (2, 0, 1, 3)).reshape(pad, -1)
        gate_col = info[0][:, None]
        prod_col = info[1] + info[2]
        pre_gate = jnp.dot(x_in, wg, preferred_element_type=f32)
        pre_up = jnp.dot(x_in, wu, preferred_element_type=f32)
        back_grad = lax.dot_general(c_in, wd, (((1,), (1,)), ((), ())), preferred_element_type=f32)
        sig = jax.nn.sigmoid(pre_gate)
        active = pre_gate * sig
        hidden = (active * pre_up).astype(bf16)
        terms = jnp.sum(hidden.astype(f32) * back_grad, axis=1)
        scaled = gate_col * back_grad
        d_gate = (scaled * pre_up * sig * (1.0 + pre_gate * (1.0 - sig))).astype(bf16)
        d_up = (scaled * active).astype(bf16)
        s_cot = (gate_col * c_in.astype(f32)).astype(bf16)
        kept.append((x_in, d_gate, d_up, hidden, s_cot))
        coef = prod_col * terms
        sign = (labels[None, :] == here).astype(f32) - (
            labels[None, :].astype(f32) == info[3][:, None]
        ).astype(f32)
        lmat = coef[:, None] * sign
        l_hi = lmat.astype(bf16)
        l_lo = (lmat - l_hi.astype(f32)).astype(bf16)
        rr = lax.dot_general(
            jnp.concatenate([l_hi, l_lo], axis=1), x_in, (((0,), (0,)), ((), ())), preferred_element_type=f32
        )
        rr = rr[:experts] + rr[experts:]
        chunk = width // total
        target = (ep * tp_count + tp) ^ jnp.arange(total)
        spot = (tp ^ (target // ep_count)) * ep_count + target % ep_count
        rr = rr.reshape(experts, total, chunk)[:, spot]
        rr = jnp.transpose(rr, (1, 0, 2)).reshape(experts, BLOCKS, tp_count, experts * chunk)
        rr = jnp.transpose(rr, (1, 0, 2, 3))
        contract = (((1,), (1,)), ((), ()))
        dx = lax.dot_general(d_gate, wg, contract, preferred_element_type=f32)
        dx = (dx + lax.dot_general(d_up, wu, contract, preferred_element_type=f32)).astype(bf16)
        kp = len(piece)
        dx = dx.reshape(BLOCKS, kp, cap, tp_count, quarter)
        gt = jnp.broadcast_to(
            jnp.pad(terms.reshape(BLOCKS, kp, 1, 1, cap), ((0, 0),) * 4 + ((0, quarter - cap),)),
            (BLOCKS, kp, 1, tp_count, quarter),
        ).astype(bf16)
        kept[-1] = kept[-1] + (rr, gt, dx)
    router_all = sum(k[5] for k in kept)
    for piece, k in zip(pieces, kept):
        gt, dx = k[6], k[7]
        kp = len(piece)
        rrow = router_all[:, piece[0] : piece[0] + kp][:, :, None]
        rrow = jnp.pad(rrow, ((0, 0),) * 4 + ((0, quarter - rrow.shape[-1]),)).astype(bf16)
        extra = jnp.concatenate([gt, rrow, jnp.zeros((BLOCKS, kp, pad - 2, tp_count, quarter), bf16)], axis=2)
        full = jnp.concatenate([dx, extra], axis=2)
        full = jnp.transpose(full, (3, 0, 1, 2, 4)).reshape(2, 2, BLOCKS, kp, cap + pad, quarter)
        gained = swap(full[:, 1], cbit)
        summed = full[:, 0].astype(f32) + gained.astype(f32)
        send = jnp.where(core == 0, summed[1], summed[:, 1]).astype(bf16)
        keep = jnp.where(core == 0, summed[0], summed[:, 0])
        keep = keep + mixed(send, ybit, xbit).astype(f32)
        last = keep[0] + mixed(keep[1].astype(bf16), xbit, ybit).astype(f32)
        last = last.astype(bf16)
        for n, j in enumerate(piece):
            backs[j] = last[n] if j == 0 else swap(last[n], zbit * j)
    contract_rows = (((0,), (0,)), ((), ()))

    def weight_grad(a, b):
        left = jnp.concatenate([k[a] for k in kept], axis=0)
        right = jnp.concatenate([k[b] for k in kept], axis=0)
        return lax.dot_general(left, right, contract_rows, preferred_element_type=f32).astype(bf16)

    grad_gate = weight_grad(0, 1).reshape(tp_count, quarter, hid)[turn].reshape(width, hid)
    grad_up = weight_grad(0, 2).reshape(tp_count, quarter, hid)[turn].reshape(width, hid)
    grad_down = weight_grad(3, 4).reshape(hid, tp_count, quarter)[:, turn].reshape(hid, width)
    back = jnp.stack(backs)
    routed = lax.dot_general(
        place.reshape(-1, rows), back[:, :cap].reshape(-1, quarter), contract_rows, preferred_element_type=f32
    )
    gate_slot = back[:, cap, :cap]
    per = jnp.einsum("jc,jct->jt", gate_slot, place, preferred_element_type=f32)
    gate_grad = jnp.stack(
        [jnp.sum(jnp.where(routes[None, :, k] == near[:, None], per, 0.0), axis=0) for k in range(top)], axis=1
    )
    router_grad = jnp.sum(back[:, cap + 1, : width // total * experts].astype(f32), axis=0)
    router_grad = router_grad.reshape(experts, width // total).T
    lead = product * (gate_grad[:, 0] - gate_grad[:, 1])
    logit_grad = (picked[:, 0] - picked[:, 1]) * lead[:, None]
    router_cols = lax.dynamic_slice_in_dim(router, tp * quarter, quarter, 0).astype(f32)
    token_grad = (routed + jnp.dot(logit_grad, router_cols.T, precision=highest)).astype(bf16)
    return (token_grad, gate_grad, grad_gate[None], grad_up[None], grad_down[None], router_grad)


def fits(mesh):
    experts = mesh.shape["ep"] // BLOCKS
    return mesh.shape["tp"] == 4 and experts * BLOCKS == mesh.shape["ep"] and experts & (experts - 1) == 0


def solution(mesh):
    placed = (
        P("ep", None),
        P("ep", None),
        P("ep", None),
        P(),
        P("ep", None, "tp"),
        P("ep", None, "tp"),
        P("ep", "tp", None),
    )
    return jax.shard_map(
        fast_shards if fits(mesh) else shards,
        mesh=mesh,
        in_specs=placed,
        out_specs=(
            P("ep", "tp"),
            P("ep", None),
            P("ep", None, "tp"),
            P("ep", None, "tp"),
            P("ep", "tp", None),
            P(("ep", "tp"), None),
        ),
        check_vma=False,
    )
```

```python
import jax
import jax.numpy as jnp
from jax import lax
from jax.experimental import pallas as pl
from jax.experimental.pallas import tpu as pltpu
from jax.sharding import PartitionSpec as P

BLOCKS = 2


def build_slots(block_routes, experts, capacity):
    flat_routes = block_routes.reshape(-1)
    labels = jnp.arange(experts, dtype=jnp.int32)
    hit_mask = (flat_routes[None, :] == labels[:, None]).astype(jnp.int32)
    rank_in = jnp.cumsum(hit_mask, axis=1, dtype=jnp.int32) - 1
    slot_ids = jnp.arange(capacity, dtype=jnp.int32)
    assigned = (hit_mask[:, None, :] == 1) & (rank_in[:, None, :] == slot_ids[None, :, None])
    return assigned.astype(jnp.float32)


def gate_pair(tokens, routes, router, experts):
    logits = jnp.dot(tokens, router, preferred_element_type=jnp.float32)
    labels = jnp.arange(experts, dtype=jnp.int32)
    picked = (routes[:, :, None] == labels[None, None, :]).astype(jnp.float32)
    chosen = jnp.sum(picked * logits[:, None, :], axis=2)
    margin = chosen[:, 0] - chosen[:, 1]
    weights = jnp.stack([jax.nn.sigmoid(margin), jax.nn.sigmoid(-margin)], axis=1)
    return (picked, weights)


def logit_grads(picked, weights, gate_grad):
    lead_grad = weights[:, 0] * weights[:, 1] * (gate_grad[:, 0] - gate_grad[:, 1])
    pair_grad = jnp.stack([lead_grad, -lead_grad], axis=1)
    return jnp.sum(picked * pair_grad[:, :, None], axis=1)


def expert_grads(rows_in, cot_in, gate_in, gate_weight, up_weight, down_weight):
    pre_gate = jnp.dot(rows_in, gate_weight, preferred_element_type=jnp.float32)
    pre_up = jnp.dot(rows_in, up_weight, preferred_element_type=jnp.float32)
    back_grad = lax.dot_general(
        cot_in, down_weight, (((1,), (1,)), ((), ())), preferred_element_type=jnp.float32
    )
    sig_gate = jax.nn.sigmoid(pre_gate)
    active = pre_gate * sig_gate
    hidden = (active * pre_up).astype(jnp.bfloat16)
    gate_terms = jnp.sum(hidden.astype(jnp.float32) * back_grad, axis=1)
    gate_col = gate_in.astype(jnp.float32)[:, None]
    scaled_back = gate_col * back_grad
    d_gate = (scaled_back * pre_up * sig_gate * (1.0 + pre_gate * (1.0 - sig_gate))).astype(
        jnp.bfloat16
    )
    d_up = (scaled_back * active).astype(jnp.bfloat16)
    scaled_cot = (gate_col * cot_in.astype(jnp.float32)).astype(jnp.bfloat16)
    contract_rows = (((0,), (0,)), ((), ()))
    grad_gate = lax.dot_general(
        rows_in, d_gate, contract_rows, preferred_element_type=jnp.float32
    ).astype(jnp.bfloat16)
    grad_up = lax.dot_general(
        rows_in, d_up, contract_rows, preferred_element_type=jnp.float32
    ).astype(jnp.bfloat16)
    grad_down = lax.dot_general(
        hidden, scaled_cot, contract_rows, preferred_element_type=jnp.float32
    ).astype(jnp.bfloat16)
    return (d_gate, d_up, gate_terms, grad_gate, grad_up, grad_down)


def spread_slabs(packed, experts, slab_count):
    widened = jnp.broadcast_to(packed[:, None], (experts, BLOCKS) + packed.shape[1:])
    return widened.reshape((slab_count,) + packed.shape[1:])


def shards(tokens, cotangent, routes, router, w_gate, w_up, w_down):
    highest = lax.Precision.HIGHEST
    ep_count = lax.axis_size("ep")
    tp_count = lax.axis_size("tp")
    experts = ep_count // BLOCKS
    tok_rows, width = tokens.shape
    top_count = routes.shape[1]
    capacity = 3 * tok_rows * top_count // (2 * experts)
    col_width = width // tp_count
    tp_index = lax.axis_index("tp")
    picked, weights = gate_pair(tokens, routes, router, experts)
    assigned = build_slots(routes, experts, capacity)
    per_token = jnp.sum(assigned.reshape(experts, capacity, tok_rows, top_count), axis=3)
    token_map = per_token.astype(jnp.bfloat16)
    gate_send = weights.astype(jnp.bfloat16)
    gate_slots = jnp.einsum(
        "ecj,j->ec", assigned, gate_send.astype(jnp.float32).reshape(-1), precision=highest
    ).astype(jnp.bfloat16)
    gate_out = spread_slabs(gate_slots, experts, ep_count)

    def pack_rows(source):
        packed = jnp.einsum(
            "ect,td->ecd", token_map, source, preferred_element_type=jnp.float32
        ).astype(jnp.bfloat16)
        return spread_slabs(packed, experts, ep_count)

    tok_part = lax.dynamic_slice_in_dim(tokens, tp_index * col_width, col_width, 1)
    cot_part = lax.dynamic_slice_in_dim(cotangent, tp_index * col_width, col_width, 1)
    recv_part, recv_cot_part, recv_gate = (
        lax.all_to_all(pack_rows(tok_part), "ep", split_axis=0, concat_axis=0, tiled=True),
        lax.all_to_all(pack_rows(cot_part), "ep", split_axis=0, concat_axis=0, tiled=True),
        lax.all_to_all(gate_out, "ep", split_axis=0, concat_axis=0, tiled=True),
    )
    recv_rows, recv_cot = (
        lax.all_gather(recv_part, "tp", axis=2, tiled=True),
        lax.all_gather(recv_cot_part, "tp", axis=2, tiled=True),
    )
    rows_in = recv_rows.reshape(-1, width)
    cot_in = recv_cot.reshape(-1, width)
    gate_in = recv_gate.reshape(-1)
    d_gate, d_up, gate_terms, grad_gate, grad_up, grad_down = expert_grads(
        rows_in, cot_in, gate_in, w_gate[0], w_up[0], w_down[0]
    )
    contract_hidden = (((1,), (1,)), ((), ()))
    partial_dx = lax.dot_general(
        d_gate, w_gate[0], contract_hidden, preferred_element_type=jnp.float32
    )
    partial_dx = partial_dx + lax.dot_general(
        d_up, w_up[0], contract_hidden, preferred_element_type=jnp.float32
    )
    summed_dx = lax.psum_scatter(
        partial_dx.reshape(ep_count, capacity, width).astype(jnp.bfloat16),
        "tp",
        scatter_dimension=2,
        tiled=True,
    ).astype(jnp.float32)
    gate_sums = lax.psum(gate_terms.reshape(ep_count, capacity), "tp")
    back_dx, back_gate = (
        lax.all_to_all(
            summed_dx.astype(jnp.bfloat16), "ep", split_axis=0, concat_axis=0, tiled=True
        ).astype(summed_dx.dtype),
        lax.all_to_all(
            gate_sums.astype(jnp.bfloat16), "ep", split_axis=0, concat_axis=0, tiled=True
        ).astype(gate_sums.dtype),
    )
    slab_dx = jnp.sum(back_dx.reshape(experts, BLOCKS, capacity, col_width), axis=1)
    routed_dx = jnp.einsum("ect,ecd->td", per_token, slab_dx, precision=highest)
    slab_gate = jnp.sum(back_gate.reshape(experts, BLOCKS, capacity), axis=1)
    gate_grad = jnp.einsum("ecj,ec->j", assigned, slab_gate, precision=highest).reshape(
        tok_rows, top_count
    )
    logit_grad = logit_grads(picked, weights, gate_grad)
    router_cols = lax.dynamic_slice_in_dim(router, tp_index * col_width, col_width, 0).astype(
        jnp.float32
    )
    token_grad = (routed_dx + jnp.dot(logit_grad, router_cols.T, precision=highest)).astype(
        jnp.bfloat16
    )
    seg_rows = tok_rows // tp_count
    own_rows = lax.dynamic_slice_in_dim(tokens, tp_index * seg_rows, seg_rows, 0).astype(
        jnp.float32
    )
    own_logit = lax.dynamic_slice_in_dim(logit_grad, tp_index * seg_rows, seg_rows, 0)
    router_grad = lax.psum_scatter(
        jnp.dot(own_rows.T, own_logit, precision=highest),
        ("ep", "tp"),
        scatter_dimension=0,
        tiled=True,
    )
    return (token_grad, gate_grad, grad_gate[None], grad_up[None], grad_down[None], router_grad)

def dot_of(a, b, ca, cb):
    return lax.dot_general(a, b, (((ca,), (cb,)), ((), ())), preferred_element_type=jnp.float32)


def as_column(row):
    n = row.shape[1]
    same = lax.broadcasted_iota(jnp.int32, (n, n), 0) == lax.broadcasted_iota(jnp.int32, (n, n), 1)
    return jnp.sum(jnp.where(same, row, 0.0), axis=1, keepdims=True)


def as_row(column):
    n = column.shape[0]
    same = lax.broadcasted_iota(jnp.int32, (n, n), 0) == lax.broadcasted_iota(jnp.int32, (n, n), 1)
    return jnp.sum(jnp.where(same, column, 0.0), axis=0, keepdims=True)


def fast_shards(tokens, cotangent, routes, router, w_gate, w_up, w_down):
    f32, bf16, i32 = jnp.float32, jnp.bfloat16, jnp.int32
    axes = ("ep", "tp")
    ep_count = lax.axis_size("ep")
    tp_count = lax.axis_size("tp")
    total = ep_count * tp_count
    experts = ep_count // BLOCKS
    rows, width = tokens.shape
    top = routes.shape[1]
    cap = 3 * rows * top // (2 * experts)
    quarter = width // tp_count
    hid = w_gate.shape[2]
    chunk = width // total
    pad = -(-(1 + experts) // 8) * 8
    tall = cap + pad
    vmem = pl.BlockSpec(memory_space=pltpu.VMEM)
    anywhere = pl.BlockSpec(memory_space=pl.ANY)

    def near_memory(values):
        return [pltpu.with_memory_space_constraint(v, pltpu.VMEM) for v in values]

    def call(body, name, args, outs, flops, mib, scratch=(), far=0):
        near = len(outs) - far
        return pl.pallas_call(
            body,
            out_shape=[pltpu.VMEM(*o) for o in outs[:near]] + [jax.ShapeDtypeStruct(*o) for o in outs[near:]],
            in_specs=[vmem] * len(args),
            out_specs=[vmem] * near + [anywhere] * far,
            scratch_shapes=list(scratch),
            compiler_params=pltpu.CompilerParams(vmem_limit_bytes=mib << 20),
            cost_estimate=pl.CostEstimate(flops=int(flops), bytes_accessed=1 << 20, transcendentals=0),
            name=name,
        )(*near_memory(args))

    def swap(value, bits):
        return lax.ppermute(value, axes, [(i, i ^ bits) for i in range(total)])

    def mixed(value, bits_even, bits_odd):
        return lax.ppermute(
            value, axes, [(i, i ^ (bits_odd if i % 2 else bits_even)) for i in range(total)]
        )

    cbit, ybit, xbit, zbit = 1, 2, tp_count, tp_count * BLOCKS

    def pack_body(tok_ref, cot_ref, route_ref, router_ref, *outs):
        packed, place_ref, product_ref, first_ref = outs[:experts], outs[experts], outs[experts + 1], outs[experts + 2]
        tp = lax.axis_index("tp")
        here = lax.axis_index("ep") // BLOCKS
        logits = dot_of(tok_ref[...], router_ref[...], 1, 1)
        r0 = as_column(route_ref[0:1, :].astype(f32)).astype(i32)
        r1 = as_column(route_ref[1:2, :].astype(f32)).astype(i32)
        lane = lax.broadcasted_iota(i32, (rows, experts), 1)
        c0 = jnp.sum(jnp.where(lane == r0, logits, 0.0), axis=1, keepdims=True)
        c1 = jnp.sum(jnp.where(lane == r1, logits, 0.0), axis=1, keepdims=True)
        w0, w1 = jax.nn.sigmoid(c0 - c1), jax.nn.sigmoid(c1 - c0)
        product = w0 * w1
        product_ref[...] = jnp.broadcast_to(product, product_ref.shape)
        wide = lax.broadcasted_iota(i32, first_ref.shape, 1)
        first_ref[...] = jnp.where(wide == 0, r0, r1)
        near = here ^ lane
        hit = (near == r0) | (near == r1)
        below = lax.broadcasted_iota(i32, (rows, rows), 1) <= lax.broadcasted_iota(i32, (rows, rows), 0)
        rank = dot_of(below.astype(bf16), hit.astype(bf16), 1, 0)
        rank = jnp.where(hit, rank - 1.0, -1.0)
        slot = lax.broadcasted_iota(i32, (rows, rows), 1).astype(f32)
        kind = lax.broadcasted_iota(i32, (rows, 128), 1)
        hi = product.astype(bf16).astype(f32)
        lo = product - hi
        spot = pl.multiple_of(tp * quarter, quarter)
        tok = tok_ref[:, pl.ds(spot, quarter)]
        cot = cot_ref[:, pl.ds(spot, quarter)]
        for j in range(experts):
            place = (rank[:, j : j + 1] == slot).astype(f32).astype(bf16)
            place_ref[:, j * rows : (j + 1) * rows] = place
            first = r0 == (here ^ j)
            gate = jnp.where(first, w0, w1)
            other = jnp.where(first, r1, r0).astype(f32)
            meta = jnp.where(
                kind == 0, gate, jnp.where(kind == 1, hi, jnp.where(kind == 2, lo, jnp.where(kind == 3, other, 0.0)))
            ).astype(bf16)
            packed[j][0:cap, 0:quarter] = dot_of(place, tok, 0, 0)[0:cap].astype(bf16)
            packed[j][0:cap, quarter:] = dot_of(place, cot, 0, 0)[0:cap].astype(bf16)
            packed[j][cap:, :] = jnp.zeros((pad, 2 * quarter), bf16)
            packed[j][cap : cap + 8, 0:rows] = dot_of(meta, place, 0, 0)[0:8].astype(bf16)

    outs = call(
        pack_body,
        "pack",
        (tokens, cotangent, routes.T, router.T),
        [((tall, 2 * quarter), bf16)] * experts + [((rows, experts * rows), bf16), ((rows, 128), f32), ((rows, 128), i32)],
        4 * rows * rows * quarter * experts,
        24,
    )
    packed, place, product, named = outs[:experts], outs[experts], outs[experts + 1], outs[experts + 2]

    half = experts // 2
    pieces = [list(range(half)), list(range(half, experts))]
    slots = quarter // (2 * chunk)

    def order(blocks):
        own, side, over, diag, town, tside, tover, tdiag = blocks
        return [[own, side], [town, tside], [over, diag], [tover, tdiag]]

    def rows_of(pair, kp, base):
        return jnp.concatenate(
            [ref[n, 0:cap, base : base + quarter] for ref in pair for n in range(kp)], axis=0
        )

    def gates_of(own, side, kp, kind):
        return jnp.concatenate(
            [as_column(ref[n, cap + kind : cap + kind + 1, 0:cap].astype(f32)) for ref in (own, side) for n in range(kp)],
            axis=0,
        )

    def forward(blocks, kp, weights):
        n = BLOCKS * kp * cap

        def body(*refs):
            quarters = order(refs[:8])
            wg_ref, wu_ref, wd_ref, x_ref, s_ref, hid_ref, dg_ref, du_ref, term_ref, sum_ref, c_ref = refs[8:]
            tp = lax.axis_index("tp")
            here = lax.axis_index("ep") // BLOCKS
            gate = gates_of(refs[0], refs[1], kp, 0)
            for r in range(tp_count):
                spot = pl.multiple_of((tp ^ r) * quarter, quarter)
                x_ref[:, pl.ds(spot, quarter)] = rows_of(quarters[r], kp, 0)
                cot = rows_of(quarters[r], kp, quarter)
                c_ref[:, pl.ds(spot, quarter)] = cot
                s_ref[:, pl.ds(spot, quarter)] = (gate * cot.astype(f32)).astype(bf16)
            term = jnp.zeros((n, 1), f32)
            for h in range(2):
                cols = slice(h * hblock, (h + 1) * hblock)
                pre_gate = dot_of(x_ref[...], wg_ref[:, cols], 1, 0)
                pre_up = dot_of(x_ref[...], wu_ref[:, cols], 1, 0)
                back = dot_of(c_ref[...], wd_ref[cols, :], 1, 1)
                sig = jax.nn.sigmoid(pre_gate)
                active = pre_gate * sig
                hidden = (active * pre_up).astype(bf16)
                hid_ref[:, cols] = hidden
                term += jnp.sum(hidden.astype(f32) * back, axis=1, keepdims=True)
                scaled = gate * back
                dg_ref[:, cols] = (scaled * pre_up * sig * (1.0 + pre_gate * (1.0 - sig))).astype(bf16)
                du_ref[:, cols] = (scaled * active).astype(bf16)
            term_ref[...] = jnp.broadcast_to(term, (n, 128))
            prod = gates_of(refs[0], refs[1], kp, 1) + gates_of(refs[0], refs[1], kp, 2)
            other = gates_of(refs[0], refs[1], kp, 3)
            lane = lax.broadcasted_iota(i32, (n, 128), 1)
            name = (lane % pad - 1).astype(f32)
            sign = jnp.where(name == here.astype(f32), 1.0, 0.0) - jnp.where(name == other, 1.0, 0.0)
            full = jnp.where(lane < 2 * pad, (prod * term) * sign, 0.0)
            upper = full.astype(bf16)
            lower = (full - upper.astype(f32)).astype(bf16)
            got = dot_of(jnp.where(lane < pad, upper, lower), x_ref[...], 0, 0)
            sum_ref[...] = got[0:pad] + got[pad : 2 * pad]

        return call(
            body,
            "forward",
            (*blocks, *weights),
            [((n, width), bf16)] * 2 + [((n, hid), bf16)] * 3 + [((n, 128), f32), ((pad, width), f32)],
            6 * n * width * hid,
            24,
            [pltpu.VMEM((n, width), bf16)],
        )

    def input_grads(d_gate, d_up, terms, sums, weights, piece, flip):
        kp = len(piece)
        final = piece is pieces[-1]
        others = [j for j in range(experts) if j not in piece]

        def body(*refs):
            dg_ref, du_ref, term_ref, wg_ref, wu_ref = refs[:5]
            sum_refs, out_ref = refs[5:-1], refs[-1]
            ep, tp = lax.axis_index("ep"), lax.axis_index("tp")
            core = (tp % 2) ^ flip
            term = term_ref[:, 0:1]
            top_row = lax.broadcasted_iota(i32, (pad, 128), 0) == 0
            for dy in range(2):
                r = 2 * dy + flip
                spot = pl.multiple_of((tp ^ r) * quarter, quarter)
                dx = dot_of(dg_ref[...], wg_ref[pl.ds(spot, quarter), :], 1, 1)
                dx += dot_of(du_ref[...], wu_ref[pl.ds(spot, quarter), :], 1, 1)
                dx = dx.astype(bf16)
                for b in range(BLOCKS):
                    k = jnp.where(core == 0, 2 * dy + b, 2 * b + dy)

                    def total_of(j):
                        target = (ep * tp_count + tp) ^ ((j * BLOCKS + b) * tp_count + r)
                        at = pl.multiple_of((target // 2) * (2 * chunk), 2 * chunk)
                        found = sum_refs[0][:, pl.ds(at, 2 * chunk)]
                        for ref in sum_refs[1:]:
                            found += ref[:, pl.ds(at, 2 * chunk)]
                        return found

                    for m, j in enumerate(piece):
                        g = (b * kp + m) * cap
                        out_ref[k, m, 0:cap, :] = dx[g : g + cap]
                        extra = jnp.pad(as_row(term[g : g + cap]), ((0, 0), (0, 128 - cap)))
                        extra = jnp.where(top_row, extra, total_of(j) if final else 0.0)
                        out_ref[k, m, cap:, :] = jnp.zeros((pad, quarter), bf16)
                        out_ref[k, m, cap:, 0 : 2 * chunk] = extra.astype(bf16)
                        if final:
                            for s, o in enumerate(others[m::kp]):
                                lanes = slice((s + 1) * 2 * chunk, (s + 2) * 2 * chunk)
                                out_ref[k, m, cap:, lanes] = total_of(o).astype(bf16)

        return call(
            body,
            "input_grads",
            (d_gate, d_up, terms, *weights[:2], *(sums if final else ())),
            [((4, kp, tall, quarter), bf16)],
            2 * BLOCKS * kp * cap * width * hid,
            16,
        )[0]

    hblock = hid // 2
    weights = (w_gate[0], w_up[0], w_down[0])
    kept, backs, sums, router_parts = [], [None] * experts, [], []
    for piece in pieces:
        kp = len(piece)
        own = jnp.stack([packed[j] if j == 0 else swap(packed[j], zbit * j) for j in piece])
        side = swap(own, xbit)
        over = swap(own, ybit)
        core = lax.axis_index("tp") % 2
        diag = mixed(jnp.where(core == 0, side, over), ybit, xbit)
        blocks = [own, side, over, diag] + [swap(v, cbit) for v in (own, side, over, diag)]
        x_in, s_cot, hidden, d_gate, d_up, terms, part = forward(blocks, kp, weights)
        sums.append(part)
        send = input_grads(d_gate, d_up, terms, sums, weights, piece, 1)
        gained = swap(send, cbit)
        keep = input_grads(d_gate, d_up, terms, sums, weights, piece, 0)
        summed = keep.astype(f32) + gained.astype(f32)
        first = mixed(summed[2:].astype(bf16), ybit, xbit)
        both = summed[:2] + first.astype(f32)
        last = both[0] + mixed(both[1].astype(bf16), xbit, ybit).astype(f32)
        last = last.astype(bf16)
        for m, j in enumerate(piece):
            backs[j] = last[m] if j == 0 else swap(last[m], zbit * j)
        if piece is pieces[-1]:
            others = [j for j in range(experts) if j not in piece]
            for m in range(kp):
                for s, o in enumerate(others[m::kp]):
                    value = last[m, cap:, (s + 1) * 2 * chunk : (s + 2) * 2 * chunk]
                    router_parts.append(value if o == 0 else swap(value, zbit * o))
        kept.append((x_in, s_cot, hidden, d_gate, d_up))

    def weight_body(*refs):
        acts = [refs[5 * p : 5 * p + 5] for p in range(len(pieces))]
        outs, bufs, sems = refs[-7:-4], refs[-4:-1], refs[-1]
        hidden, d_gate, d_up = (jnp.concatenate([a[i][...] for a in acts], axis=0) for i in range(2, 5))
        copies = []
        for r in range(tp_count):
            cols = slice(r * quarter, (r + 1) * quarter)
            tok = jnp.concatenate([a[0][:, cols] for a in acts], axis=0)
            cot = jnp.concatenate([a[1][:, cols] for a in acts], axis=0)
            bufs[0][cols, :] = dot_of(tok, d_gate, 0, 0).astype(bf16)
            bufs[1][cols, :] = dot_of(tok, d_up, 0, 0).astype(bf16)
            bufs[2][:, cols] = dot_of(hidden, cot, 0, 0).astype(bf16)
            for i in range(3):
                where = (cols, slice(None)) if i < 2 else (slice(None), cols)
                copy = pltpu.make_async_copy(bufs[i].at[where], outs[i].at[where], sems.at[3 * r + i])
                copy.start()
                copies.append(copy)
        for copy in copies:
            copy.wait()

    grad_gate, grad_up, grad_down = call(
        weight_body,
        "weight_grads",
        [v for k in kept for v in k],
        [((width, hid), bf16), ((width, hid), bf16), ((hid, width), bf16)],
        6 * BLOCKS * experts * cap * width * hid,
        40,
        [
            pltpu.VMEM((width, hid), bf16),
            pltpu.VMEM((width, hid), bf16),
            pltpu.VMEM((hid, width), bf16),
            pltpu.SemaphoreType.DMA((3 * tp_count,)),
        ],
        far=3,
    )

    def finish_body(*refs):
        back, parts = refs[:experts], refs[experts : experts + len(router_parts)]
        place_ref, product_ref, named_ref, router_ref, tok_out, gate_out, router_out = refs[experts + len(router_parts) :]
        tp = lax.axis_index("tp")
        here = lax.axis_index("ep") // BLOCKS
        r0, r1 = named_ref[:, 0:1], named_ref[:, 1:2]
        routed = jnp.zeros((rows, quarter), f32)
        g0 = jnp.zeros((rows, 1), f32)
        g1 = jnp.zeros((rows, 1), f32)
        sums = jnp.zeros((pad, 2 * chunk), f32)
        for j in range(experts):
            place = place_ref[:, j * rows : j * rows + cap]
            routed += dot_of(place, back[j][0:cap, :], 1, 0)
            per = jnp.sum(place.astype(f32) * back[j][cap : cap + 1, 0:cap].astype(f32), axis=1, keepdims=True)
            g0 += jnp.where(r0 == (here ^ j), per, 0.0)
            g1 += jnp.where(r1 == (here ^ j), per, 0.0)
            if j in pieces[-1]:
                sums += back[j][cap:, 0 : 2 * chunk].astype(f32)
        for part in parts:
            sums += part[...].astype(f32)
        lane2 = lax.broadcasted_iota(i32, (rows, top), 1)
        gate_out[...] = jnp.where(lane2 == 0, g0, g1)
        lead = product_ref[:, 0:1] * (g0 - g1)
        lane = lax.broadcasted_iota(i32, (rows, experts), 1)
        lgrad = jnp.where(lane == r0, lead, 0.0) - jnp.where(lane == r1, lead, 0.0)
        upper = lgrad.astype(bf16)
        lower = (lgrad - upper.astype(f32)).astype(bf16)
        cols = router_ref[:, pl.ds(pl.multiple_of(tp * quarter, quarter), quarter)]
        routed += dot_of(upper, cols, 1, 0) + dot_of(lower, cols, 1, 0)
        tok_out[...] = routed.astype(bf16)
        router_out[...] = jnp.where(tp % 2 == 0, sums[1 : 1 + experts, 0:chunk], sums[1 : 1 + experts, chunk : 2 * chunk])

    args = (*backs, *router_parts, place, product, named, router.T)
    token_grad, gate_grad, router_sum = pl.pallas_call(
        finish_body,
        out_shape=[
            jax.ShapeDtypeStruct((rows, quarter), bf16),
            jax.ShapeDtypeStruct((rows, top), f32),
            jax.ShapeDtypeStruct((experts, chunk), f32),
        ],
        in_specs=[vmem] * len(args),
        out_specs=[vmem] * 3,
        compiler_params=pltpu.CompilerParams(vmem_limit_bytes=16 << 20),
        name="finish",
    )(*near_memory(args))
    return (token_grad, gate_grad, grad_gate[None], grad_up[None], grad_down[None], router_sum.T)


def fits(mesh):
    experts = mesh.shape["ep"] // BLOCKS
    return mesh.shape["tp"] == 4 and experts * BLOCKS == mesh.shape["ep"] and experts & (experts - 1) == 0


def solution(mesh):
    placed = (
        P("ep", None),
        P("ep", None),
        P("ep", None),
        P(),
        P("ep", None, "tp"),
        P("ep", None, "tp"),
        P("ep", "tp", None),
    )
    return jax.shard_map(
        fast_shards if fits(mesh) else shards,
        mesh=mesh,
        in_specs=placed,
        out_specs=(
            P("ep", "tp"),
            P("ep", None),
            P("ep", None, "tp"),
            P("ep", None, "tp"),
            P("ep", "tp", None),
            P(("ep", "tp"), None),
        ),
        check_vma=False,
    )
```
